256 devices in a mesh: ep: 64 (over z, x, core), tp: 4 (over y).
Axes of the slice: x: 4, y: 4, z: 8, core: 2. Of those that a mesh axis runs over, the one named last changes fastest.
Arguments:
- tokens: bfloat16 [16384, 2048], P('ep'), may hold values from -6 to 6
- norm_gain: float32 [2048], replicated, may hold values from 0.1 to 1.9
- expert_ids: int32 [16384, 4], P('ep'), may hold values from 0 to 63, all different within a row; in each aligned block of 256 rows (0 to 255, 256 to 511, ...) at most 32 rows name the same one
- route_weights: float32 [16384, 4], P('ep'), may hold values from 0.05 to 1
- gate_weight: bfloat16 [64, 2048, 2048], P('ep', None, 'tp'), as said below
- up_weight: bfloat16 [64, 2048, 2048], P('ep', None, 'tp'), as said below
- down_weight: bfloat16 [64, 2048, 2048], P('ep', 'tp'), may hold values from -0.125 to 0.125
Outputs:
- mixed: bfloat16 [16384, 2048], P('ep', 'tp')
The draws below stay inside these ranges and needn't reach their ends.
Inputs may be any that keep to these rules, and one draw needn't show every extreme that they name: `expert_ids`: each row names 4 different experts. In the rows of one device no expert is named by more than 32 rows, and in every draw some expert is named by exactly 32 rows of some device. `gate_weight`: independent entries of mean zero, drawn for each expert separately. `up_weight`: independent entries of mean zero, drawn for each expert separately.
All inputs are finite; a program needn't handle non-finite values.
Results may differ from the reference program's by a relative error of at most 0.014.
Values may be sent and summed in bfloat16 or wider, within the bound.
A program may use at most 128 MiB of HBM per device.

```python
import math
import jax
import jax.numpy as jnp
import numpy as np
from jax import lax

D = 2048
FF = 2048
TOP = 4
TOK_DEV = 256
EXPERTS = 64
CAP = 32
TOKENS = 16384
N_TP = 4


def draw_gate_weight(key, part):
    factor = 1.0
    values = jax.random.normal(jax.random.fold_in(key, 11), (EXPERTS, D, FF), jnp.float32)
    return (values * (factor / D ** 0.5)).astype(jnp.bfloat16)


def draw_up_weight(key, part):
    factor = 1.0
    values = jax.random.normal(jax.random.fold_in(key, 23), (EXPERTS, D, FF), jnp.float32)
    return (values * (factor / D ** 0.5)).astype(jnp.bfloat16)


def levels(stream_key, shape, split, smallest, largest):
    gain, own = 1.0, jax.random.fold_in(stream_key, 6)
    for dim, blocks in split:
        draws = jnp.exp(jax.random.uniform(jax.random.fold_in(own, dim), (blocks,), jnp.float32, smallest / len(split), largest / len(split)))
        gain = gain * jnp.repeat(draws, shape[dim] // blocks).reshape([-1 if axis == dim else 1 for axis in range(len(shape))])
    return gain


def deal_out(own_key, own, number, rows, count, top, most, lean):
    sequence = jax.random.permutation(own_key, count)
    heavy_load, ordinary = portions_of(count, rows * top, most, lean, True), portions_of(count, rows * top, most, lean, False)
    places = jnp.arange(count)

    def named(lengths, rotation):
        used = int((lengths > 0).sum())
        fixed = max(1, used // 4)
        moved = fixed + (places - fixed + rotation * (used - fixed)) % max(1, count - fixed)
        return jnp.zeros((count,), jnp.int32).at[sequence[jnp.where(places < fixed, places, moved)]].set(jnp.asarray(lengths, jnp.int32))

    lengths = jnp.where(number % 4 == 0, named(heavy_load, number // 4), named(ordinary, number - number // 4 - 1))
    mixed = jax.random.permutation(jax.random.fold_in(own, 3), count)
    source_of, sink = mixed[0:count // 2 * 2:2], mixed[1:count // 2 * 2:2]
    slack = jnp.minimum(lengths[source_of] - 1, most - lengths[sink]) // 2
    slack = jnp.where((source_of == sequence[0]) | (sink == sequence[0]) | (lengths[sink] == 0), 0, jnp.maximum(slack, 0))
    moved = jax.random.randint(jax.random.fold_in(own, 4), (count // 2,), 0, 1 << 20) % (slack + 1)
    lengths = lengths.at[source_of].add(-moved).at[sink].add(moved)
    labels = jnp.searchsorted(jnp.cumsum(lengths), jnp.arange(rows * top), side="right").astype(jnp.int32)
    listing = labels.reshape(top, rows).T
    listing = listing[jax.random.permutation(jax.random.fold_in(own, 1), rows)]
    rotation = jax.random.randint(jax.random.fold_in(own, 2), (rows, 1), 0, top)
    return jnp.take_along_axis(listing, (jnp.arange(top)[None, :] + rotation) % top, axis=1)


def portions_of(number_of, total, reach, slope, full):
    portions = [(1 << 20) // math.isqrt(standing ** slope) + 1 for standing in range(1, number_of + 1)]
    largest = reach if full else min(reach, max(-(-total // number_of), total * portions[0] // sum(portions)))
    least = 1 if total - largest >= number_of - 1 else 0
    holding, rest = [largest] + [least] * (number_of - 1), total - largest - least * (number_of - 1)
    while rest > 0:
        movable = [i for i in range(1, number_of) if holding[i] < largest] or [i for i in range(1, number_of) if holding[i] < reach]
        pool, remaining = sum([portions[i] for i in movable]), rest
        for i in movable:
            extra = min(reach - holding[i], max(1, remaining * portions[i] // pool), rest)
            holding[i] = holding[i] + extra
            rest = rest - extra
    return np.array(holding)


def scatter_about(stream_key, dims, scale, reach, shards=(), held_as=jnp.bfloat16):
    values = scale * jax.random.normal(stream_key, dims, jnp.float32)
    if shards:
        values = values * levels(stream_key, dims, shards, -0.22, 0.18)
    return jnp.clip(values, -reach, reach).astype(held_as)


def setup_inputs(seed: int = 0) -> dict:
    key_of = jax.random.split(jax.random.key(seed), 8)
    tokens = scatter_about(key_of[0], (TOKENS, D), 1.0, 6.0, ((0, 64),))
    norm_gain = jnp.clip(1.0 + 0.18 * jax.random.normal(key_of[1], (D,), jnp.float32), 0.1, 1.9)
    expert_ids_keys = jax.random.split(jax.random.fold_in(key_of[2], 1), TOKENS // TOK_DEV)
    expert_ids_turns = jax.random.permutation(jax.random.fold_in(key_of[2], 3), TOKENS // TOK_DEV)
    expert_ids = jax.vmap(lambda own, number: deal_out(jax.random.fold_in(key_of[2], 2), own, number, TOK_DEV, EXPERTS, TOP, CAP, 2))(expert_ids_keys, expert_ids_turns).reshape((TOKENS, TOP))
    route_weights = jnp.clip(0.05 + 0.95 * jax.random.uniform(key_of[3], (TOKENS, TOP), jnp.float32) ** levels(key_of[3], (TOKENS, TOP), ((0, 64),), -0.2, 0.2), 0.05, 1.0)
    gate_weight = draw_gate_weight(jax.random.fold_in(key_of[7], 71), 0)
    up_weight = draw_up_weight(jax.random.fold_in(key_of[7], 71), 0)
    down_weight = scatter_about(key_of[6], (EXPERTS, FF, D), FF ** -0.5, 0.125, ((0, 64), (1, 4)))
    return dict(tokens=tokens, norm_gain=norm_gain, expert_ids=expert_ids, route_weights=route_weights, gate_weight=gate_weight, up_weight=up_weight, down_weight=down_weight)


def reference(tokens, norm_gain, expert_ids, route_weights, gate_weight, up_weight, down_weight):
    values = tokens.astype(jnp.float32)
    scale = lax.rsqrt(lax.optimization_barrier(jnp.mean(values * values, axis=1, keepdims=True)) + 1e-06)
    normed = (values * scale * norm_gain[None, :]).astype(jnp.bfloat16)
    blocks = TOKENS // TOK_DEV
    pairs_dev = TOK_DEV * TOP
    flat = expert_ids.reshape(blocks, pairs_dev)
    onehot = (flat[:, :, None] == jnp.arange(EXPERTS, dtype=jnp.int32)[None, None, :]).astype(jnp.int32)
    before = jnp.cumsum(onehot, axis=1) - onehot
    slot = lax.optimization_barrier(jnp.sum(before * onehot, axis=2))
    source = jnp.arange(blocks, dtype=jnp.int32)[:, None]
    position = (slot + source * CAP).reshape(-1).astype(jnp.int32)
    pair_tok = (source * TOK_DEV + jnp.arange(pairs_dev, dtype=jnp.int32)[None, :] // TOP).reshape(-1).astype(jnp.int32)
    expert_flat = flat.reshape(-1).astype(jnp.int32)
    rows = blocks * CAP
    tok_table = jnp.zeros((EXPERTS, rows), jnp.int32).at[expert_flat, position].set(pair_tok)
    weight_table = jnp.zeros((EXPERTS, rows), jnp.float32).at[expert_flat, position].set(route_weights.reshape(-1))

    def one_expert(total, index):
        chosen = normed[tok_table[index]]
        gate = jnp.dot(chosen, gate_weight[index], preferred_element_type=jnp.float32)
        upper = jnp.dot(chosen, up_weight[index], preferred_element_type=jnp.float32)
        gate = jnp.minimum(gate, 7.0)
        upper = jnp.clip(upper, -7.0, 7.0)
        hidden = ((upper + 1.0) * (gate * jax.nn.sigmoid(1.702 * gate))).astype(jnp.bfloat16)
        blocked = hidden.reshape(rows, N_TP, FF // N_TP).astype(jnp.float32)
        down_blocks = down_weight[index].reshape(N_TP, FF // N_TP, D).astype(jnp.float32)
        partial_value = jnp.einsum('rpf,pfd->rpd', blocked, down_blocks).astype(jnp.bfloat16)
        expert_out = lax.optimization_barrier(jnp.sum(partial_value.astype(jnp.float32), axis=1)).astype(jnp.bfloat16)
        total = total.at[tok_table[index]].add(weight_table[index][:, None] * expert_out.astype(jnp.float32))
        return (total, None)
    start = jnp.zeros((TOKENS, D), jnp.float32)
    total, unused = lax.scan(one_expert, start, jnp.arange(EXPERTS, dtype=jnp.int32))
    return total.astype(jnp.bfloat16)
```

```python
import jax
import jax.numpy as jnp
from jax import lax
from jax.experimental import pallas as pl
from jax.experimental.pallas import tpu as pltpu
from jax.sharding import PartitionSpec as P

MESH = pl.DeviceIdType.MESH
NZ = 8
NJ = 8
NY = 4
TOK = 256
CAP = 32
W = 2048
Q = 512
ROWS = NJ * CAP
META = 16
R, L = 0, 1
A, B = 0, 1
HALF = NZ // 2
PARTS = 2
BF = jnp.bfloat16
F32 = jnp.float32


def top_hop(direction, chunk):
    return HALF if direction == chunk else HALF - 1


SCHEDULE = (
    "D00", "D01", "Y00", "Z1100", "Z0100", "Z1101", "D10", "Z0101", "Z1110", "D70", "Y10", "Z1111",
    "Z0200", "D11", "Y70", "Z1200", "Z1201", "D20", "Z0201", "Z1210", "Z0300", "D60", "Y20", "Z1211",
    "Z0301", "D50", "Y60", "Z0111", "Z0110", "D21", "Z0400", "Z0401", "Y50", "D40", "Z0211", "Z1300",
    "D71", "Z1311", "Z0210", "Z1301", "Z1310", "Y40", "D30", "Z0311", "D61", "Z1411", "Z1410", "D41",
    "Y30", "Z0310", "D51", "D31", "F40", "F50", "F30", "G40", "F60", "G50", "F20", "C4", "G30", "r0401",
    "r1410", "r0400", "F70", "r1411", "C5", "r1301", "r1310", "C3", "r0310", "G60", "r0300", "r1300",
    "G20", "r1311", "r0311", "F10", "C6", "r0301", "r1201", "G70", "C2", "r0200", "F00", "r1211",
    "r1200", "r0211", "r0210", "G10", "C7", "r0201", "r1210", "r1111", "G00", "C1", "r0111", "r1110",
    "r1101", "r0110", "r0101", "r1100", "r0100", "C0", "E1", "E0", "O1", "O0",
)


def kernel(
    tok_ref, gain_ref, ids_ref, rw_ref, wg_ref, wu_ref, wd_ref, out_ref,
    za, zb, xs, xf, wgu, wdn, hid, ps, yr, xs2, cr, tsum, rin, rout, exs, exr, info_ref,
    w_sem, z_s, z_r, x_s, x_r, y_s, y_r, p_s, p_r, q_s, q_r, c_s, c_r, e_s, e_r,
):
    me = lax.axis_index("ep")
    y = lax.axis_index("tp")
    z = me // NJ
    j = lax.rem(me, NJ)
    up_z = lax.rem(z + 1, NZ) * NJ + j
    down_z = lax.rem(z + NZ - 1, NZ) * NJ + j
    y_up = lax.rem(y + 1, NY)
    y_far = lax.rem(y + 2, NY)
    y_down = lax.rem(y + 3, NY)
    zdev = ((up_z, y), (down_z, y))
    ydev = ((me, y_up), (me, y_down))

    def peer(o):
        return lax.rem(j + o, NJ)

    def quarter(i):
        return pl.ds(pl.multiple_of((y, y_far, y_down, y_up)[i] * Q, Q), Q)

    weights = []
    for i in range(4):
        weights.append((wg_ref.at[0, quarter(i), :], wgu.at[pl.ds(i * Q, Q), pl.ds(0, Q)]))
        weights.append((wu_ref.at[0, quarter(i), :], wgu.at[pl.ds(i * Q, Q), pl.ds(Q, Q)]))
        weights.append((wd_ref.at[0, :, quarter(i)], wdn.at[:, pl.ds(i * Q, Q)]))
    weights = [pltpu.make_async_copy(s, d, w_sem.at[i]) for i, (s, d) in enumerate(weights)]
    for copy in weights:
        copy.start()

    barrier = pltpu.get_barrier_semaphore()
    partners = list(zdev) + list(ydev) + [(me, y_far)]
    partners += [(z * NJ + peer(o), y) for o in range(1, NJ)]
    for device in partners:
        pl.semaphore_signal(barrier, inc=1, device_id=device, device_id_type=MESH)

    sends = []

    def send(src, dst, ssem, rsem, device):
        copy = pltpu.make_async_remote_copy(
            src_ref=src, dst_ref=dst, send_sem=ssem, recv_sem=rsem,
            device_id=device, device_id_type=MESH,
        )
        copy.start()
        return copy

    def await_bytes(ref, sem):
        pltpu.make_async_copy(ref, ref, sem).wait()

    ids = ids_ref[...].astype(F32)
    expert = lax.broadcasted_iota(jnp.int32, (NZ * NJ, TOK), 0).astype(F32)
    hits = [ids[k : k + 1, :] == expert for k in range(4)]
    named = jnp.where(hits[0] | hits[1] | hits[2] | hits[3], 1.0, 0.0).astype(BF)
    earlier = lax.broadcasted_iota(jnp.int32, (TOK, TOK), 0) < lax.broadcasted_iota(
        jnp.int32, (TOK, TOK), 1
    )
    before = jnp.dot(named, jnp.where(earlier, 1.0, 0.0).astype(BF), preferred_element_type=F32)
    info_ref[...] = jnp.zeros_like(info_ref)
    info_ref[pl.ds(0, 4), :] = ids
    for k in range(4):
        slot = jnp.sum(jnp.where(hits[k], before, 0.0), axis=0, keepdims=True)
        info_ref[pl.ds(4 + k, 1), :] = slot
    info_ref[pl.ds(8, 4), :] = rw_ref[...]
    za[0, pl.ds(TOK, META), pl.ds(0, TOK)] = info_ref[...].astype(BF)
    za[0, pl.ds(TOK, META), pl.ds(TOK, TOK)] = jnp.zeros((META, TOK), BF)

    values = tok_ref[...].astype(F32)
    scale = lax.rsqrt(jnp.mean(values * values, axis=1, keepdims=True) + 1e-06)
    for i, buf in enumerate((za, zb)):
        part = tok_ref[:, quarter(i)].astype(F32) * scale * gain_ref[:, quarter(i)]
        buf[0, pl.ds(0, TOK), :] = part.astype(BF)

    pl.semaphore_wait(barrier, len(partners))

    def piece(chunk, part):
        size = (TOK + META, TOK)[chunk]
        cut = (TOK // 2 + META, TOK // 2)[chunk]
        return pl.ds(0, cut) if part == 0 else pl.ds(cut, size - cut)

    def z_send(direction, hop, chunk, part):
        buf = (za, zb)[chunk]
        here = (-hop if direction == R else hop) % NZ
        there = (-(hop + 1) if direction == R else hop + 1) % NZ
        rows = piece(chunk, part)
        sends.append(
            send(
                buf.at[here, rows], buf.at[there, rows],
                z_s.at[direction, hop, chunk, part], z_r.at[direction, hop, chunk, part],
                zdev[direction],
            )
        )

    def z_step(direction, hop, chunk, part):
        buf = (za, zb)[chunk]
        slot = (-hop if direction == R else hop) % NZ
        await_bytes(buf.at[slot, piece(chunk, part)], z_r.at[direction, hop - 1, chunk, part])
        if hop < top_hop(direction, chunk):
            z_send(direction, hop, chunk, part)

    for chunk in (A, B):
        for part in range(PARTS):
            for direction in (R, L):
                z_send(direction, 0, chunk, part)

    base = (z * ROWS).astype(F32)

    def places(b):
        info = za[b, pl.ds(TOK, META), pl.ds(0, TOK)].astype(F32)
        at = lax.broadcasted_iota(jnp.int32, (ROWS, TOK), 0).astype(F32) + base
        return info, [info[k : k + 1] * CAP + info[4 + k : 5 + k] == at for k in range(4)]

    def rows_of(p):
        return pl.ds(pl.multiple_of(p * CAP, CAP), CAP)

    def exchange(src, dst, ssem, rsem):
        for o in range(1, NJ):
            p = peer(o)
            send(src.at[rows_of(p), :], dst.at[rows_of(j), :], ssem, rsem, (z * NJ + p, y))
        dst[rows_of(j), :] = src[rows_of(j), :]

    def await_exchange(dst, rsem):
        await_bytes(dst.at[pl.ds(0, ROWS - CAP), :], rsem)

    def cols(i):
        return pl.ds(i * Q, Q)

    def dispatch(b, chunk):
        info, at = places(b)
        pick = jnp.where(at[0] | at[1] | at[2] | at[3], 1.0, 0.0).astype(BF)
        block = (za, zb)[chunk][b, pl.ds(0, TOK), :]
        xs[b, chunk] = jnp.dot(pick, block, preferred_element_type=F32).astype(BF)
        exchange(xs.at[b, chunk], xf.at[b, :, cols(chunk)], x_s.at[b, chunk], x_r.at[b, chunk])

    def spread(b):
        await_exchange(xf.at[b, :, cols(A)], x_r.at[b, A])
        for side in range(2):
            sends.append(
                send(
                    xf.at[b, :, cols(A)], xf.at[b, :, cols(2 + side)],
                    y_s.at[side, b], y_r.at[side, b], ydev[side],
                )
            )

    def experts(b):
        await_exchange(xf.at[b, :, cols(B)], x_r.at[b, B])
        for side in range(2):
            await_bytes(xf.at[b, :, cols(2 + side)], y_r.at[side, b])
        rows = xf[b]
        for n in range(2):
            gate = jnp.dot(rows, wgu[:, pl.ds(n * 256, 256)], preferred_element_type=F32)
            upper = jnp.dot(rows, wgu[:, pl.ds(Q + n * 256, 256)], preferred_element_type=F32)
            gate = jnp.minimum(gate, 7.0)
            upper = jnp.clip(upper, -7.0, 7.0)
            hid[:, pl.ds(n * 256, 256)] = (
                (upper + 1.0) * (gate * jax.nn.sigmoid(1.702 * gate))
            ).astype(BF)
        for i in (2, 3, 1, 0):
            part = jnp.dot(hid[...], wdn[:, cols(i)], preferred_element_type=F32)
            ps[b, i] = part.astype(BF)
            if i >= 2:
                side = 3 - i
                sends.append(
                    send(
                        ps.at[b, i], yr.at[side, b],
                        p_s.at[side, b], p_r.at[side, b], ydev[side],
                    )
                )
            elif i == 1:
                exchange(ps.at[b, 1], cr.at[b, B], q_s.at[b, B], q_r.at[b, B])

    def give_back(b):
        for side in range(2):
            await_bytes(yr.at[side, b], p_r.at[side, b])
        total = ps[b, 0].astype(F32) + yr[0, b].astype(F32) + yr[1, b].astype(F32)
        xs2[b] = total.astype(BF)
        exchange(xs2.at[b], cr.at[b, A], q_s.at[b, A], q_r.at[b, A])

    def combine(b):
        for chunk in (A, B):
            await_exchange(cr.at[b, chunk], q_r.at[b, chunk])
        info, at = places(b)
        weight = jnp.zeros((ROWS, TOK), F32)
        for k in range(4):
            weight = jnp.where(at[k], info[8 + k : 9 + k], weight)
        weight = weight.astype(BF)
        for chunk in (A, B):
            tsum[b, chunk] = lax.dot_general(
                weight, cr[b, chunk], (((0,), (0,)), ((), ())), preferred_element_type=F32
            )

    def span(part):
        return pl.ds(part * (TOK // PARTS), TOK // PARTS)

    def reduce_step(direction, hop, chunk, part):
        b = (hop if direction == R else -hop) % NZ
        value = tsum[b, chunk, span(part), :]
        if hop < top_hop(direction, chunk):
            came = rin.at[direction, hop, chunk, span(part), :]
            await_bytes(came, c_r.at[direction, hop, chunk, part])
            value = value + came[...].astype(F32)
        src = rout.at[direction, hop - 1, chunk, span(part), :]
        src[...] = value.astype(BF)
        sends.append(
            send(
                src, rin.at[direction, hop - 1, chunk, span(part), :],
                c_s.at[direction, hop - 1, chunk, part], c_r.at[direction, hop - 1, chunk, part],
                zdev[direction],
            )
        )

    def arrived(chunk, part):
        total = tsum[0, chunk, span(part), :]
        for direction in (R, L):
            came = rin.at[direction, 0, chunk, span(part), :]
            await_bytes(came, c_r.at[direction, 0, chunk, part])
            total = total + came[...].astype(F32)
        return total

    def finish_far(part):
        exs[span(part), :] = arrived(B, part).astype(BF)
        sends.append(
            send(
                exs.at[span(part), :], exr.at[span(part), :],
                e_s.at[part], e_r.at[part], (me, y_far),
            )
        )

    def finish_own(part):
        own = arrived(A, part)
        await_bytes(exr.at[span(part), :], e_r.at[part])
        out_ref[span(part), :] = (own + exr[span(part), :].astype(F32)).astype(BF)

    waiting = list(weights)
    for name in SCHEDULE:
        arg = [int(d) for d in name[1:]]
        if name[0] == "F":
            while waiting:
                waiting.pop().wait()
        if name[0] in "YFG":
            arg = arg[:1]
        {
            "Z": z_step, "D": dispatch, "Y": spread, "F": experts, "G": give_back,
            "C": combine, "r": reduce_step, "E": finish_far, "O": finish_own,
        }[name[0]](*arg)

    for copy in sends:
        copy.wait_send()
    for b in range(NZ):
        for chunk in (A, B):
            await_exchange(xs.at[b, chunk], x_s.at[b, chunk])
        await_exchange(xs2.at[b], q_s.at[b, A])
        await_exchange(ps.at[b, 1], q_s.at[b, B])


def per_device(tokens, norm_gain, expert_ids, route_weights, gate_weight, up_weight, down_weight):
    vmem = pl.BlockSpec(memory_space=pltpu.VMEM)
    hbm = pl.BlockSpec(memory_space=pl.ANY)
    dma = pltpu.SemaphoreType.DMA
    return pl.pallas_call(
        kernel,
        out_shape=jax.ShapeDtypeStruct((TOK, Q), BF),
        in_specs=[vmem, vmem, vmem, vmem, hbm, hbm, hbm],
        out_specs=vmem,
        scratch_shapes=[
            pltpu.VMEM((NZ, TOK + META, Q), BF),
            pltpu.VMEM((NZ, TOK, Q), BF),
            pltpu.VMEM((NZ, 2, ROWS, Q), BF),
            pltpu.VMEM((NZ, ROWS, W), BF),
            pltpu.VMEM((W, 2 * Q), BF),
            pltpu.VMEM((Q, W), BF),
            pltpu.VMEM((ROWS, Q), BF),
            pltpu.VMEM((NZ, 4, ROWS, Q), BF),
            pltpu.VMEM((2, NZ, ROWS, Q), BF),
            pltpu.VMEM((NZ, ROWS, Q), BF),
            pltpu.VMEM((NZ, 2, ROWS, Q), BF),
            pltpu.VMEM((NZ, 2, TOK, Q), F32),
            pltpu.VMEM((2, HALF, 2, TOK, Q), BF),
            pltpu.VMEM((2, HALF, 2, TOK, Q), BF),
            pltpu.VMEM((TOK, Q), BF),
            pltpu.VMEM((TOK, Q), BF),
            pltpu.VMEM((META, TOK), F32),
            dma((12,)),
            dma((2, HALF, 2, PARTS)), dma((2, HALF, 2, PARTS)),
            dma((NZ, 2)), dma((NZ, 2)),
            dma((2, NZ)), dma((2, NZ)),
            dma((2, NZ)), dma((2, NZ)),
            dma((NZ, 2)), dma((NZ, 2)),
            dma((2, HALF, 2, PARTS)), dma((2, HALF, 2, PARTS)),
            dma((PARTS,)), dma((PARTS,)),
        ],
        compiler_params=pltpu.CompilerParams(
            collective_id=0, has_side_effects=True, vmem_limit_bytes=67_000_000
        ),
        name="moe",
    )(
        tokens, norm_gain.reshape(1, W), expert_ids.T, route_weights.T,
        gate_weight, up_weight, down_weight,
    )


def solution(mesh):
    in_specs = (
        P("ep", None),
        P(),
        P("ep", None),
        P("ep", None),
        P("ep", None, "tp"),
        P("ep", None, "tp"),
        P("ep", "tp", None),
    )
    out_specs = P("ep", "tp")
    return jax.shard_map(
        per_device, mesh=mesh, in_specs=in_specs, out_specs=out_specs, check_vma=False
    )
```

```python
import jax
import jax.numpy as jnp
from jax import lax
from jax.experimental import pallas as pl
from jax.experimental.pallas import tpu as pltpu
from jax.sharding import PartitionSpec as P

MESH = pl.DeviceIdType.MESH
NZ = 8
NJ = 8
NY = 4
TOK = 256
CAP = 32
W = 2048
Q = 512
ROWS = NJ * CAP
META = 16
R, L = 0, 1
A, B = 0, 1
HALF = NZ // 2
PARTS = 2
CUTS = 1
SUB = CAP // CUTS
PIECE = ROWS // CUTS
BF = jnp.bfloat16
F32 = jnp.float32


def top_hop(direction, chunk):
    return HALF if direction == chunk else HALF - 1


SCHEDULE = (
    "D00", "Z1100", "D01", "Z1101", "Z0100", "Z0101", "D70", "Y00", "Z1110", "D10", "Z1111", "Y70",
    "D11", "Y10", "Z0200", "Z0201", "D60", "Z1201", "Z0300", "Z1200", "Z0110", "D20", "Z1210", "Y60",
    "Z0301", "D50", "Z0111", "Z1301", "D71", "Y20", "Z1211", "D21", "Z0401", "Z1310", "Z0210", "Z1300",
    "Z0400", "D40", "Y50", "Z0211", "D30", "Z1311", "D61", "Y40", "Z1410", "Z1411", "Z0310", "Z0311",
    "D51", "D41", "D31", "Y30", "F50", "F40", "F30", "F20", "F60", "C41", "r1410", "r1411", "C31",
    "r0311", "G40", "C51", "G50", "r0310", "C21", "F10", "r0211", "r1310", "G30", "C40", "r0210",
    "r1311", "C61", "r0401", "C50", "r1300", "r0400", "F70", "r1211", "G20", "C11", "r1210", "r1301",
    "C30", "r0110", "r0301", "G60", "F00", "r0300", "C71", "r1111", "G10", "r0111", "r1110", "C60",
    "C20", "r0201", "C01", "r0200", "r1201", "G70", "r1200", "C10", "E1", "r0101", "C70", "r1101",
    "r0100", "E0", "G00", "r1100", "C00", "O1", "O0",
)


def kernel(
    tok_hbm, gain_ref, ids_ref, rw_ref, wg_ref, wu_ref, wd_ref, own_hbm, far_hbm,
    tok_ref, own_ref, za, zb, xs, xf, wgu, wdn, hid, ps, yr, xs2, cr, tsum, rin, rout, exs, info_ref,
    t_sem, o_sem, w_sem, z_s, z_r, x_s, x_r, y_s, y_r, p_s, p_r, q_s, q_r, c_s, c_r, e_s, e_r,
):
    me = lax.axis_index("ep")
    y = lax.axis_index("tp")
    z = me // NJ
    j = lax.rem(me, NJ)
    up_z = lax.rem(z + 1, NZ) * NJ + j
    down_z = lax.rem(z + NZ - 1, NZ) * NJ + j
    y_up = lax.rem(y + 1, NY)
    y_far = lax.rem(y + 2, NY)
    y_down = lax.rem(y + 3, NY)
    zdev = ((up_z, y), (down_z, y))
    ydev = ((me, y_up), (me, y_down))

    def peer(o):
        return lax.rem(j + o, NJ)

    def quarter(i):
        return pl.ds(pl.multiple_of((y, y_far, y_down, y_up)[i] * Q, Q), Q)

    tokens = pltpu.make_async_copy(tok_hbm, tok_ref, t_sem)
    tokens.start()

    barrier = pltpu.get_barrier_semaphore()
    partners = list(zdev) + list(ydev) + [(me, y_far)]
    partners += [(z * NJ + peer(o), y) for o in range(1, NJ)]
    for device in partners:
        pl.semaphore_signal(barrier, inc=1, device_id=device, device_id_type=MESH)

    weights = []
    for i in range(4):
        weights.append((wg_ref.at[0, quarter(i), :], wgu.at[pl.ds(i * Q, Q), pl.ds(0, Q)]))
        weights.append((wu_ref.at[0, quarter(i), :], wgu.at[pl.ds(i * Q, Q), pl.ds(Q, Q)]))
        weights.append((wd_ref.at[0, :, quarter(i)], wdn.at[:, pl.ds(i * Q, Q)]))
    weights = [pltpu.make_async_copy(s, d, w_sem.at[i]) for i, (s, d) in enumerate(weights)]

    sends = []

    def send(src, dst, ssem, rsem, device):
        copy = pltpu.make_async_remote_copy(
            src_ref=src, dst_ref=dst, send_sem=ssem, recv_sem=rsem,
            device_id=device, device_id_type=MESH,
        )
        copy.start()
        return copy

    def await_bytes(ref, sem):
        pltpu.make_async_copy(ref, ref, sem).wait()

    ids = ids_ref[...].astype(F32)
    expert = lax.broadcasted_iota(jnp.int32, (NZ * NJ, TOK), 0).astype(F32)
    hits = [ids[k : k + 1, :] == expert for k in range(4)]
    named = jnp.where(hits[0] | hits[1] | hits[2] | hits[3], 1.0, 0.0).astype(BF)
    earlier = lax.broadcasted_iota(jnp.int32, (TOK, TOK), 0) < lax.broadcasted_iota(
        jnp.int32, (TOK, TOK), 1
    )
    before = jnp.dot(named, jnp.where(earlier, 1.0, 0.0).astype(BF), preferred_element_type=F32)
    info_ref[...] = jnp.zeros_like(info_ref)
    info_ref[pl.ds(0, 4), :] = ids
    for k in range(4):
        slot = jnp.sum(jnp.where(hits[k], before, 0.0), axis=0, keepdims=True)
        info_ref[pl.ds(4 + k, 1), :] = slot
    info_ref[pl.ds(8, 4), :] = rw_ref[...]
    za[0, pl.ds(TOK, META), pl.ds(0, TOK)] = info_ref[...].astype(BF)
    za[0, pl.ds(TOK, META), pl.ds(TOK, TOK)] = jnp.zeros((META, TOK), BF)

    tokens.wait()
    for copy in weights:
        copy.start()
    values = tok_ref[...].astype(F32)
    scale = lax.rsqrt(jnp.mean(values * values, axis=1, keepdims=True) + 1e-06)
    for i, buf in enumerate((za, zb)):
        part = tok_ref[:, quarter(i)].astype(F32) * scale * gain_ref[:, quarter(i)]
        buf[0, pl.ds(0, TOK), :] = part.astype(BF)

    pl.semaphore_wait(barrier, len(partners))

    def piece(chunk, part):
        size = (TOK + META, TOK)[chunk]
        step = TOK // PARTS
        first = size - TOK
        return pl.ds(0, step + first) if part == 0 else pl.ds(first + part * step, step)

    def z_send(direction, hop, chunk, part):
        buf = (za, zb)[chunk]
        here = (-hop if direction == R else hop) % NZ
        there = (-(hop + 1) if direction == R else hop + 1) % NZ
        rows = piece(chunk, part)
        sends.append(
            send(
                buf.at[here, rows], buf.at[there, rows],
                z_s.at[direction, hop, chunk, part], z_r.at[direction, hop, chunk, part],
                zdev[direction],
            )
        )

    def z_step(direction, hop, chunk, part):
        buf = (za, zb)[chunk]
        slot = (-hop if direction == R else hop) % NZ
        await_bytes(buf.at[slot, piece(chunk, part)], z_r.at[direction, hop - 1, chunk, part])
        if hop < top_hop(direction, chunk):
            z_send(direction, hop, chunk, part)

    for chunk in (A, B):
        for part in range(PARTS):
            for direction in (R, L):
                z_send(direction, 0, chunk, part)

    base = (z * ROWS).astype(F32)

    def places(b):
        info = za[b, pl.ds(TOK, META), pl.ds(0, TOK)].astype(F32)
        row = lax.broadcasted_iota(jnp.int32, (ROWS, TOK), 0)
        row = lax.rem(row, PIECE) // SUB * CAP + row // PIECE * SUB + lax.rem(row, SUB)
        at = row.astype(F32) + base
        return info, [info[k : k + 1] * CAP + info[4 + k : 5 + k] == at for k in range(4)]

    def rows_of(p):
        return pl.ds(pl.multiple_of(p * SUB, SUB), SUB)

    def exchange(src, dst, ssem, rsem):
        for o in range(1, NJ):
            p = peer(o)
            send(src.at[rows_of(p), :], dst.at[rows_of(j), :], ssem, rsem, (z * NJ + p, y))
        dst[rows_of(j), :] = src[rows_of(j), :]

    def await_exchange(dst, rsem):
        await_bytes(dst.at[pl.ds(0, PIECE - SUB), :], rsem)

    def cut(i):
        return pl.ds(i * PIECE, PIECE)

    def cols(i):
        return pl.ds(i * Q, Q)

    def dispatch(b, chunk):
        info, at = places(b)
        pick = jnp.where(at[0] | at[1] | at[2] | at[3], 1.0, 0.0).astype(BF)
        block = (za, zb)[chunk][b, pl.ds(0, TOK), :]
        xs[b, chunk] = jnp.dot(pick, block, preferred_element_type=F32).astype(BF)
        for i in range(CUTS):
            exchange(
                xs.at[b, chunk, cut(i)], xf.at[b, cut(i), cols(chunk)],
                x_s.at[b, chunk, i], x_r.at[b, chunk, i],
            )

    def spread(b, i):
        await_exchange(xf.at[b, cut(i), cols(A)], x_r.at[b, A, i])
        for side in range(2):
            sends.append(
                send(
                    xf.at[b, cut(i), cols(A)], xf.at[b, cut(i), cols(2 + side)],
                    y_s.at[side, b, i], y_r.at[side, b, i], ydev[side],
                )
            )

    def experts(b, i):
        await_exchange(xf.at[b, cut(i), cols(B)], x_r.at[b, B, i])
        for side in range(2):
            await_bytes(xf.at[b, cut(i), cols(2 + side)], y_r.at[side, b, i])
        rows = xf[b, cut(i), :]
        for n in range(2):
            gate = jnp.dot(rows, wgu[:, pl.ds(n * 256, 256)], preferred_element_type=F32)
            upper = jnp.dot(rows, wgu[:, pl.ds(Q + n * 256, 256)], preferred_element_type=F32)
            gate = jnp.minimum(gate, 7.0)
            upper = jnp.clip(upper, -7.0, 7.0)
            hid[:, pl.ds(n * 256, 256)] = (
                (upper + 1.0) * (gate * jax.nn.sigmoid(1.702 * gate))
            ).astype(BF)
        for q in (2, 3, 1, 0):
            part = jnp.dot(hid[...], wdn[:, cols(q)], preferred_element_type=F32)
            ps[b, q, cut(i), :] = part.astype(BF)
            if q >= 2:
                side = 3 - q
                sends.append(
                    send(
                        ps.at[b, q, cut(i)], yr.at[side, b, cut(i)],
                        p_s.at[side, b, i], p_r.at[side, b, i], ydev[side],
                    )
                )
            elif q == 1:
                exchange(
                    ps.at[b, 1, cut(i)], cr.at[b, B, cut(i)], q_s.at[b, B, i], q_r.at[b, B, i]
                )

    def give_back(b, i):
        total = ps[b, 0, cut(i), :].astype(F32)
        for side in range(2):
            await_bytes(yr.at[side, b, cut(i)], p_r.at[side, b, i])
            total = total + yr[side, b, cut(i), :].astype(F32)
        xs2[b, cut(i), :] = total.astype(BF)
        exchange(xs2.at[b, cut(i)], cr.at[b, A, cut(i)], q_s.at[b, A, i], q_r.at[b, A, i])

    def combine(b, chunk):
        for i in range(CUTS):
            await_exchange(cr.at[b, chunk, cut(i)], q_r.at[b, chunk, i])
        info, at = places(b)
        weight = jnp.zeros((ROWS, TOK), F32)
        for k in range(4):
            weight = jnp.where(at[k], info[8 + k : 9 + k], weight)
        tsum[b, chunk] = lax.dot_general(
            weight.astype(BF), cr[b, chunk], (((0,), (0,)), ((), ())), preferred_element_type=F32
        )

    def span(part):
        return pl.ds(part * (TOK // PARTS), TOK // PARTS)

    def reduce_step(direction, hop, chunk, part):
        b = (hop if direction == R else -hop) % NZ
        value = tsum[b, chunk, span(part), :]
        if hop < top_hop(direction, chunk):
            came = rin.at[direction, hop, chunk, span(part), :]
            await_bytes(came, c_r.at[direction, hop, chunk, part])
            value = value + came[...].astype(F32)
        src = rout.at[direction, hop - 1, chunk, span(part), :]
        src[...] = value.astype(BF)
        sends.append(
            send(
                src, rin.at[direction, hop - 1, chunk, span(part), :],
                c_s.at[direction, hop - 1, chunk, part], c_r.at[direction, hop - 1, chunk, part],
                zdev[direction],
            )
        )

    def arrived(chunk, part):
        total = tsum[0, chunk, span(part), :]
        for direction in (R, L):
            came = rin.at[direction, 0, chunk, span(part), :]
            await_bytes(came, c_r.at[direction, 0, chunk, part])
            total = total + came[...].astype(F32)
        return total

    def finish_far(part):
        exs[span(part), :] = arrived(B, part).astype(BF)
        sends.append(
            send(
                exs.at[span(part), :], far_hbm.at[span(part), :],
                e_s.at[part], e_r.at[part], (me, y_far),
            )
        )

    results = []

    def finish_own(part):
        own_ref[span(part), :] = arrived(A, part)
        copy = pltpu.make_async_copy(
            own_ref.at[span(part), :], own_hbm.at[span(part), :], o_sem.at[part]
        )
        copy.start()
        results.append(copy)

    waiting = list(weights)
    for name in SCHEDULE:
        arg = [int(d) for d in name[1:]]
        if name[0] == "F":
            while waiting:
                waiting.pop().wait()
        {
            "Z": z_step, "D": dispatch, "Y": spread, "F": experts, "G": give_back,
            "C": combine, "r": reduce_step, "E": finish_far, "O": finish_own,
        }[name[0]](*arg)

    for part in range(PARTS):
        await_bytes(far_hbm.at[span(part), :], e_r.at[part])
    for copy in results:
        copy.wait()
    for copy in sends:
        copy.wait_send()
    for b in range(NZ):
        for i in range(CUTS):
            for chunk in (A, B):
                await_exchange(xs.at[b, chunk, cut(i)], x_s.at[b, chunk, i])
            await_exchange(xs2.at[b, cut(i)], q_s.at[b, A, i])
            await_exchange(ps.at[b, 1, cut(i)], q_s.at[b, B, i])


def per_device(tokens, norm_gain, expert_ids, route_weights, gate_weight, up_weight, down_weight):
    vmem = pl.BlockSpec(memory_space=pltpu.VMEM)
    hbm = pl.BlockSpec(memory_space=pl.ANY)
    dma = pltpu.SemaphoreType.DMA
    own, far = pl.pallas_call(
        kernel,
        out_shape=[jax.ShapeDtypeStruct((TOK, Q), F32), jax.ShapeDtypeStruct((TOK, Q), BF)],
        in_specs=[hbm, vmem, vmem, vmem, hbm, hbm, hbm],
        out_specs=[hbm, hbm],
        scratch_shapes=[
            pltpu.VMEM((TOK, W), BF),
            pltpu.VMEM((TOK, Q), F32),
            pltpu.VMEM((NZ, TOK + META, Q), BF),
            pltpu.VMEM((NZ, TOK, Q), BF),
            pltpu.VMEM((NZ, 2, ROWS, Q), BF),
            pltpu.VMEM((NZ, ROWS, W), BF),
            pltpu.VMEM((W, 2 * Q), BF),
            pltpu.VMEM((Q, W), BF),
            pltpu.VMEM((PIECE, Q), BF),
            pltpu.VMEM((NZ, 4, ROWS, Q), BF),
            pltpu.VMEM((2, NZ, ROWS, Q), BF),
            pltpu.VMEM((NZ, ROWS, Q), BF),
            pltpu.VMEM((NZ, 2, ROWS, Q), BF),
            pltpu.VMEM((NZ, 2, TOK, Q), F32),
            pltpu.VMEM((2, HALF, 2, TOK, Q), BF),
            pltpu.VMEM((2, HALF, 2, TOK, Q), BF),
            pltpu.VMEM((TOK, Q), BF),
            pltpu.VMEM((META, TOK), F32),
            dma, dma((PARTS,)), dma((12,)),
            dma((2, HALF, 2, PARTS)), dma((2, HALF, 2, PARTS)),
            dma((NZ, 2, CUTS)), dma((NZ, 2, CUTS)),
            dma((2, NZ, CUTS)), dma((2, NZ, CUTS)),
            dma((2, NZ, CUTS)), dma((2, NZ, CUTS)),
            dma((NZ, 2, CUTS)), dma((NZ, 2, CUTS)),
            dma((2, HALF, 2, PARTS)), dma((2, HALF, 2, PARTS)),
            dma((PARTS,)), dma((PARTS,)),
        ],
        compiler_params=pltpu.CompilerParams(
            collective_id=0, has_side_effects=True, vmem_limit_bytes=67_000_000
        ),
        name="moe",
    )(
        tokens, norm_gain.reshape(1, W), expert_ids.T, route_weights.T,
        gate_weight, up_weight, down_weight,
    )
    return (own + far.astype(F32)).astype(BF)


def solution(mesh):
    in_specs = (
        P("ep", None),
        P(),
        P("ep", None),
        P("ep", None),
        P("ep", None, "tp"),
        P("ep", None, "tp"),
        P("ep", "tp", None),
    )
    out_specs = P("ep", "tp")
    return jax.shard_map(
        per_device, mesh=mesh, in_specs=in_specs, out_specs=out_specs, check_vma=False
    )
```

```python
import jax
import jax.numpy as jnp
from jax import lax
from jax.experimental import pallas as pl
from jax.experimental.pallas import tpu as pltpu
from jax.sharding import PartitionSpec as P

MESH = pl.DeviceIdType.MESH
NZ = 8
NJ = 8
NY = 4
TOK = 256
CAP = 32
W = 2048
Q = 512
ROWS = NJ * CAP
META = 16
R, L = 0, 1
A, B = 0, 1
HALF = NZ // 2
PARTS = 2
CUTS = 1
SUB = CAP // CUTS
PIECE = ROWS // CUTS
C = Q // PARTS
EARLY = (0, 1, NZ - 1)
BF = jnp.bfloat16
F32 = jnp.float32


def top_hop(direction, chunk):
    return HALF if direction == chunk else HALF - 1


SCHEDULE = (
    "H00", "B11", "H01", "B10", "J00", "Z1100", "Z0100", "H10", "H70", "J01", "Z0101", "H71", "D01",
    "J10", "Z0200", "Z1101", "J70", "H11", "Z1110", "Z1111", "Z0201", "D60", "D11", "J71", "B00", "B01",
    "Z1200", "J11", "Z0300", "Z0301", "D50", "Z1201", "Y60", "Z1210", "D20", "Z0111", "Z1211", "Z0110",
    "D71", "Y50", "Z0400", "Z1300", "D21", "Y20", "Z0401", "D40", "Z1310", "Z1301", "D30", "Z0211",
    "Z1311", "D31", "Z0210", "D61", "Y40", "Y30", "Z1411", "Z1410", "D41", "F20", "Z0310", "Z0311",
    "D51", "F40", "F30", "F50", "C41", "r1410", "F60", "C31", "r0310", "r0311", "r1411", "C51", "G40",
    "r1310", "F70", "C61", "C21", "r1311", "r0210", "G20", "C40", "r0401", "r0400", "r1210", "r0211",
    "G30", "F10", "G50", "r1211", "C71", "r1110", "C30", "r0300", "G60", "r0301", "C20", "r1111", "F00",
    "C50", "r1301", "C11", "r0111", "r1300", "G70", "C60", "r0110", "r0200", "r1201", "G10", "C01",
    "r0201", "r1200", "C70", "E0", "r1101", "E1", "C10", "r0100", "G00", "r1100", "r0101", "C00", "O0",
    "O1",
)


def kernel(
    tok_hbm, gain_ref, ids_ref, rw_ref, wg_ref, wu_ref, wd_ref, own_hbm, far_hbm,
    tok_ref, own_ref, za, zb, xs, xf, wgu, wdn, hid, ps, yr, xs2, cr, tsum, rin, rout, exs, info_ref,
    t_sem, o_sem, h_s, h_r, j_s, j_r, w_sem, z_s, z_r, x_s, x_r, y_s, y_r, p_s, p_r, q_s, q_r, c_s, c_r, e_s, e_r,
):
    me = lax.axis_index("ep")
    y = lax.axis_index("tp")
    z = me // NJ
    j = lax.rem(me, NJ)
    up_z = lax.rem(z + 1, NZ) * NJ + j
    down_z = lax.rem(z + NZ - 1, NZ) * NJ + j
    y_up = lax.rem(y + 1, NY)
    y_far = lax.rem(y + 2, NY)
    y_down = lax.rem(y + 3, NY)
    zdev = ((up_z, y), (down_z, y))
    ydev = ((me, y_up), (me, y_down))

    def peer(o):
        return lax.rem(j + o, NJ)

    def quarter(i):
        return pl.ds(pl.multiple_of((y, y_far, y_down, y_up)[i] * Q, Q), Q)

    halves = [pl.ds(i * (TOK // 2), TOK // 2) for i in range(2)]
    tokens = [
        pltpu.make_async_copy(tok_hbm.at[rows, :], tok_ref.at[rows, :], t_sem.at[i])
        for i, rows in enumerate(halves)
    ]
    for copy in tokens:
        copy.start()

    barrier = pltpu.get_barrier_semaphore()
    partners = list(zdev) + list(ydev) + [(me, y_far)]
    partners += [(z * NJ + peer(o), y) for o in range(1, NJ)]
    for device in partners:
        pl.semaphore_signal(barrier, inc=1, device_id=device, device_id_type=MESH)

    weights = []
    for i in range(4):
        weights.append((wg_ref.at[0, quarter(i), :], wgu.at[pl.ds(i * Q, Q), pl.ds(0, Q)]))
        weights.append((wu_ref.at[0, quarter(i), :], wgu.at[pl.ds(i * Q, Q), pl.ds(Q, Q)]))
        weights.append((wd_ref.at[0, :, quarter(i)], wdn.at[:, pl.ds(i * Q, Q)]))
    weights = [pltpu.make_async_copy(s, d, w_sem.at[i]) for i, (s, d) in enumerate(weights)]

    sends = []

    def send(src, dst, ssem, rsem, device):
        copy = pltpu.make_async_remote_copy(
            src_ref=src, dst_ref=dst, send_sem=ssem, recv_sem=rsem,
            device_id=device, device_id_type=MESH,
        )
        copy.start()
        return copy

    def await_bytes(ref, sem):
        pltpu.make_async_copy(ref, ref, sem).wait()

    ids = ids_ref[...].astype(F32)
    expert = lax.broadcasted_iota(jnp.int32, (NZ * NJ, TOK), 0).astype(F32)
    hits = [ids[k : k + 1, :] == expert for k in range(4)]
    named = jnp.where(hits[0] | hits[1] | hits[2] | hits[3], 1.0, 0.0).astype(BF)
    earlier = lax.broadcasted_iota(jnp.int32, (TOK, TOK), 0) < lax.broadcasted_iota(
        jnp.int32, (TOK, TOK), 1
    )
    before = jnp.dot(named, jnp.where(earlier, 1.0, 0.0).astype(BF), preferred_element_type=F32)
    info_ref[...] = jnp.zeros_like(info_ref)
    info_ref[pl.ds(0, 4), :] = ids
    for k in range(4):
        slot = jnp.sum(jnp.where(hits[k], before, 0.0), axis=0, keepdims=True)
        info_ref[pl.ds(4 + k, 1), :] = slot
    info_ref[pl.ds(8, 4), :] = rw_ref[...]
    za[0, 0, pl.ds(TOK, META), :] = info_ref[...].astype(BF)

    def piece(chunk, b, part):
        rows = TOK + META if (chunk, part) == (A, 0) else TOK
        return (za, zb)[chunk].at[b, part, pl.ds(0, rows), :]

    def z_send(direction, hop, chunk, part):
        here = (-hop if direction == R else hop) % NZ
        there = (-(hop + 1) if direction == R else hop + 1) % NZ
        sends.append(
            send(
                piece(chunk, here, part), piece(chunk, there, part),
                z_s.at[direction, hop, chunk, part], z_r.at[direction, hop, chunk, part],
                zdev[direction],
            )
        )

    def z_step(direction, hop, chunk, part):
        slot = (-hop if direction == R else hop) % NZ
        await_bytes(piece(chunk, slot, part), z_r.at[direction, hop - 1, chunk, part])
        if hop < top_hop(direction, chunk):
            z_send(direction, hop, chunk, part)

    def normalise(chunk, part):
        at = (y, y_far)[chunk] * Q + part * C
        cols = pl.ds(pl.multiple_of(at, C), C)
        for rows, scale in zip(halves, scales):
            value = tok_ref[rows, cols].astype(F32) * scale * gain_ref[:, cols]
            (za, zb)[chunk][0, part, rows, :] = value.astype(BF)

    scales = []
    for copy, rows in zip(tokens, halves):
        copy.wait()
        values = tok_ref[rows, :].astype(F32)
        scales.append(lax.rsqrt(jnp.mean(values * values, axis=1, keepdims=True) + 1e-06))
    for part in range(PARTS):
        normalise(A, part)
        if part == 0:
            pl.semaphore_wait(barrier, len(partners))
        for direction in (R, L):
            z_send(direction, 0, A, part)
    for copy in weights:
        copy.start()
    for part in range(PARTS):
        normalise(B, part)

    def z_start(direction, part):
        z_send(direction, 0, B, part)

    base = (z * ROWS).astype(F32)

    def places(b):
        info = za[b, 0, pl.ds(TOK, META), :].astype(F32)
        row = lax.broadcasted_iota(jnp.int32, (ROWS, TOK), 0)
        row = lax.rem(row, PIECE) // SUB * CAP + row // PIECE * SUB + lax.rem(row, SUB)
        at = row.astype(F32) + base
        return info, [info[k : k + 1] * CAP + info[4 + k : 5 + k] == at for k in range(4)]

    def rows_of(p):
        return pl.ds(pl.multiple_of(p * SUB, SUB), SUB)

    def exchange(src, dst, ssem, rsem):
        for o in range(1, NJ):
            p = peer(o)
            send(src.at[rows_of(p), :], dst.at[rows_of(j), :], ssem, rsem, (z * NJ + p, y))
        dst[rows_of(j), :] = src[rows_of(j), :]

    def await_exchange(dst, rsem):
        await_bytes(dst.at[pl.ds(0, PIECE - SUB), :], rsem)

    def cut(i):
        return pl.ds(i * PIECE, PIECE)

    def cols(i):
        return pl.ds(i * Q, Q)

    def picked(b, chunk, parts):
        info, at = places(b)
        pick = jnp.where(at[0] | at[1] | at[2] | at[3], 1.0, 0.0).astype(BF)
        for part in parts:
            block = (za, zb)[chunk][b, part, pl.ds(0, TOK), :]
            xs[b, chunk, :, fine(part)] = jnp.dot(
                pick, block, preferred_element_type=F32
            ).astype(BF)

    def fine(part):
        return pl.ds(part * C, C)

    def dispatch(b, chunk):
        picked(b, chunk, range(PARTS))
        exchange(
            xs.at[b, chunk], xf.at[b, :, cols(chunk)], x_s.at[b, chunk, 0], x_r.at[b, chunk, 0]
        )

    def early_dispatch(b, part):
        picked(b, A, (part,))
        exchange(
            xs.at[b, A, :, fine(part)], xf.at[b, :, fine(part)], h_s.at[b, part], h_r.at[b, part]
        )

    def spread(b, i):
        await_exchange(xf.at[b, :, cols(A)], x_r.at[b, A, i])
        for side in range(2):
            sends.append(
                send(
                    xf.at[b, :, cols(A)], xf.at[b, :, cols(2 + side)],
                    y_s.at[side, b, i], y_r.at[side, b, i], ydev[side],
                )
            )

    def early_landing(b, side, part):
        return xf.at[b, :, pl.ds((2 + side) * Q + part * C, C)]

    def early_spread(b, part):
        await_exchange(xf.at[b, :, fine(part)], h_r.at[b, part])
        for side in range(2):
            sends.append(
                send(
                    xf.at[b, :, fine(part)], early_landing(b, side, part),
                    j_s.at[side, b, part], j_r.at[side, b, part], ydev[side],
                )
            )

    def experts(b, i):
        await_exchange(xf.at[b, cut(i), cols(B)], x_r.at[b, B, i])
        for side in range(2):
            if b in EARLY:
                for part in range(PARTS):
                    await_bytes(early_landing(b, side, part), j_r.at[side, b, part])
            else:
                await_bytes(xf.at[b, cut(i), cols(2 + side)], y_r.at[side, b, i])
        rows = xf[b, cut(i), :]
        for n in range(2):
            gate = jnp.dot(rows, wgu[:, pl.ds(n * 256, 256)], preferred_element_type=F32)
            upper = jnp.dot(rows, wgu[:, pl.ds(Q + n * 256, 256)], preferred_element_type=F32)
            gate = jnp.minimum(gate, 7.0)
            upper = jnp.clip(upper, -7.0, 7.0)
            hid[:, pl.ds(n * 256, 256)] = (
                (upper + 1.0) * (gate * jax.nn.sigmoid(1.702 * gate))
            ).astype(BF)
        for q in (2, 3, 1, 0):
            part = jnp.dot(hid[...], wdn[:, cols(q)], preferred_element_type=F32)
            ps[b, q, cut(i), :] = part.astype(BF)
            if q >= 2:
                side = 3 - q
                sends.append(
                    send(
                        ps.at[b, q, cut(i)], yr.at[side, b, cut(i)],
                        p_s.at[side, b, i], p_r.at[side, b, i], ydev[side],
                    )
                )
            elif q == 1:
                exchange(
                    ps.at[b, 1, cut(i)], cr.at[b, B, cut(i)], q_s.at[b, B, i], q_r.at[b, B, i]
                )

    def give_back(b, i):
        total = ps[b, 0, cut(i), :].astype(F32)
        for side in range(2):
            await_bytes(yr.at[side, b, cut(i)], p_r.at[side, b, i])
            total = total + yr[side, b, cut(i), :].astype(F32)
        xs2[b, cut(i), :] = total.astype(BF)
        exchange(xs2.at[b, cut(i)], cr.at[b, A, cut(i)], q_s.at[b, A, i], q_r.at[b, A, i])

    def combine(b, chunk):
        for i in range(CUTS):
            await_exchange(cr.at[b, chunk, cut(i)], q_r.at[b, chunk, i])
        info, at = places(b)
        weight = jnp.zeros((ROWS, TOK), F32)
        for k in range(4):
            weight = jnp.where(at[k], info[8 + k : 9 + k], weight)
        tsum[b, chunk] = lax.dot_general(
            weight.astype(BF), cr[b, chunk], (((0,), (0,)), ((), ())), preferred_element_type=F32
        )

    def span(part):
        return pl.ds(part * (TOK // PARTS), TOK // PARTS)

    def reduce_step(direction, hop, chunk, part):
        b = (hop if direction == R else -hop) % NZ
        value = tsum[b, chunk, span(part), :]
        if hop < top_hop(direction, chunk):
            came = rin.at[direction, hop, chunk, span(part), :]
            await_bytes(came, c_r.at[direction, hop, chunk, part])
            value = value + came[...].astype(F32)
        src = rout.at[direction, hop - 1, chunk, span(part), :]
        src[...] = value.astype(BF)
        sends.append(
            send(
                src, rin.at[direction, hop - 1, chunk, span(part), :],
                c_s.at[direction, hop - 1, chunk, part], c_r.at[direction, hop - 1, chunk, part],
                zdev[direction],
            )
        )

    def arrived(chunk, part):
        total = tsum[0, chunk, span(part), :]
        for direction in (R, L):
            came = rin.at[direction, 0, chunk, span(part), :]
            await_bytes(came, c_r.at[direction, 0, chunk, part])
            total = total + came[...].astype(F32)
        return total

    def finish_far(part):
        exs[span(part), :] = arrived(B, part).astype(BF)
        sends.append(
            send(
                exs.at[span(part), :], far_hbm.at[span(part), :],
                e_s.at[part], e_r.at[part], (me, y_far),
            )
        )

    results = []

    def finish_own(part):
        own_ref[span(part), :] = arrived(A, part)
        copy = pltpu.make_async_copy(
            own_ref.at[span(part), :], own_hbm.at[span(part), :], o_sem.at[part]
        )
        copy.start()
        results.append(copy)

    waiting = list(weights)
    for name in SCHEDULE:
        arg = [int(d) for d in name[1:]]
        if name[0] == "F":
            while waiting:
                waiting.pop().wait()
        {
            "Z": z_step, "D": dispatch, "Y": spread, "F": experts, "G": give_back,
            "C": combine, "r": reduce_step, "B": z_start, "H": early_dispatch, "J": early_spread, "E": finish_far, "O": finish_own,
        }[name[0]](*arg)

    for part in range(PARTS):
        await_bytes(far_hbm.at[span(part), :], e_r.at[part])
    for copy in results:
        copy.wait()
    for copy in sends:
        copy.wait_send()
    for b in range(NZ):
        for i in range(CUTS):
            if b in EARLY:
                for part in range(PARTS):
                    await_exchange(xs.at[b, A, :, fine(part)], h_s.at[b, part])
            else:
                await_exchange(xs.at[b, A], x_s.at[b, A, i])
            await_exchange(xs.at[b, B], x_s.at[b, B, i])
            await_exchange(xs2.at[b, cut(i)], q_s.at[b, A, i])
            await_exchange(ps.at[b, 1, cut(i)], q_s.at[b, B, i])


def per_device(tokens, norm_gain, expert_ids, route_weights, gate_weight, up_weight, down_weight):
    vmem = pl.BlockSpec(memory_space=pltpu.VMEM)
    hbm = pl.BlockSpec(memory_space=pl.ANY)
    dma = pltpu.SemaphoreType.DMA
    own, far = pl.pallas_call(
        kernel,
        out_shape=[jax.ShapeDtypeStruct((TOK, Q), F32), jax.ShapeDtypeStruct((TOK, Q), BF)],
        in_specs=[hbm, vmem, vmem, vmem, hbm, hbm, hbm],
        out_specs=[hbm, hbm],
        scratch_shapes=[
            pltpu.VMEM((TOK, W), BF),
            pltpu.VMEM((TOK, Q), F32),
            pltpu.VMEM((NZ, PARTS, TOK + META, C), BF),
            pltpu.VMEM((NZ, PARTS, TOK, C), BF),
            pltpu.VMEM((NZ, 2, ROWS, Q), BF),
            pltpu.VMEM((NZ, ROWS, W), BF),
            pltpu.VMEM((W, 2 * Q), BF),
            pltpu.VMEM((Q, W), BF),
            pltpu.VMEM((PIECE, Q), BF),
            pltpu.VMEM((NZ, 4, ROWS, Q), BF),
            pltpu.VMEM((2, NZ, ROWS, Q), BF),
            pltpu.VMEM((NZ, ROWS, Q), BF),
            pltpu.VMEM((NZ, 2, ROWS, Q), BF),
            pltpu.VMEM((NZ, 2, TOK, Q), F32),
            pltpu.VMEM((2, HALF, 2, TOK, Q), BF),
            pltpu.VMEM((2, HALF, 2, TOK, Q), BF),
            pltpu.VMEM((TOK, Q), BF),
            pltpu.VMEM((META, TOK), F32),
            dma((2,)), dma((PARTS,)),
            dma((NZ, PARTS)), dma((NZ, PARTS)),
            dma((2, NZ, PARTS)), dma((2, NZ, PARTS)),
            dma((12,)),
            dma((2, HALF, 2, PARTS)), dma((2, HALF, 2, PARTS)),
            dma((NZ, 2, CUTS)), dma((NZ, 2, CUTS)),
            dma((2, NZ, CUTS)), dma((2, NZ, CUTS)),
            dma((2, NZ, CUTS)), dma((2, NZ, CUTS)),
            dma((NZ, 2, CUTS)), dma((NZ, 2, CUTS)),
            dma((2, HALF, 2, PARTS)), dma((2, HALF, 2, PARTS)),
            dma((PARTS,)), dma((PARTS,)),
        ],
        compiler_params=pltpu.CompilerParams(
            collective_id=0, has_side_effects=True, vmem_limit_bytes=67_000_000
        ),
        name="moe",
    )(
        tokens, norm_gain.reshape(1, W), expert_ids.T, route_weights.T,
        gate_weight, up_weight, down_weight,
    )
    return (own + far.astype(F32)).astype(BF)


def solution(mesh):
    in_specs = (
        P("ep", None),
        P(),
        P("ep", None),
        P("ep", None),
        P("ep", None, "tp"),
        P("ep", None, "tp"),
        P("ep", "tp", None),
    )
    out_specs = P("ep", "tp")
    return jax.shard_map(
        per_device, mesh=mesh, in_specs=in_specs, out_specs=out_specs, check_vma=False
    )
```

```python
import jax
import jax.numpy as jnp
from jax import lax
from jax.experimental import pallas as pl
from jax.experimental.pallas import tpu as pltpu
from jax.sharding import PartitionSpec as P

MESH = pl.DeviceIdType.MESH
NZ = 8
NJ = 8
NY = 4
TOK = 256
CAP = 32
W = 2048
Q = 512
ROWS = NJ * CAP
META = 16
R, L = 0, 1
A, B = 0, 1
HALF = NZ // 2
PARTS = 2
CUTS = 1
SUB = CAP // CUTS
PIECE = ROWS // CUTS
C = Q // PARTS
EARLY = (0, 1, NZ - 1)
BF = jnp.bfloat16
F32 = jnp.float32


def top_hop(direction, chunk):
    return HALF if direction == chunk else HALF - 1


SCHEDULE = (
    "H00", "B11", "H01", "B10", "J00", "Z1100", "Z0100", "H10", "H70", "J01", "Z0101", "H71", "D01",
    "J10", "Z0200", "Z1101", "J70", "H11", "Z1110", "Z1111", "Z0201", "D60", "D11", "J71", "B00", "B01",
    "Z1200", "J11", "Z0300", "Z0301", "D50", "Z1201", "Y60", "Z1210", "D20", "Z0111", "Z1211", "Z0110",
    "D71", "Y50", "Z0400", "Z1300", "D21", "Y20", "Z0401", "D40", "Z1310", "Z1301", "D30", "Z0211",
    "Z1311", "D31", "Z0210", "D61", "Y40", "Y30", "Z1411", "Z1410", "D41", "F20", "Z0310", "Z0311",
    "D51", "F40", "F30", "F50", "C41", "r1410", "F60", "C31", "r0310", "r0311", "r1411", "C51", "G40",
    "r1310", "F70", "C61", "C21", "r1311", "r0210", "G20", "C40", "r0401", "r0400", "r1210", "r0211",
    "G30", "F10", "G50", "r1211", "C71", "r1110", "C30", "r0300", "G60", "r0301", "C20", "r1111", "F00",
    "C50", "r1301", "C11", "r0111", "r1300", "G70", "C60", "r0110", "r0200", "r1201", "G10", "C01",
    "r0201", "r1200", "C70", "E0", "r1101", "E1", "C10", "r0100", "G00", "r1100", "r0101", "C00", "O0",
    "O1",
)


def kernel(
    tok_hbm, gain_ref, ids_ref, rw_ref, wg_ref, wu_ref, wd_ref, own_hbm, far_hbm,
    tok_ref, own_ref, za, zb, xs, xf, wgu, wdn, hid, ps, yr, xs2, cr, tsum, rin, rout, exs, info_ref,
    t_sem, o_sem, h_s, h_r, j_s, j_r, w_sem, z_s, z_r, x_s, x_r, y_s, y_r, p_s, p_r, q_s, q_r, c_s, c_r, e_s, e_r,
):
    me = lax.axis_index("ep")
    y = lax.axis_index("tp")
    z = me // NJ
    j = lax.rem(me, NJ)
    up_z = lax.rem(z + 1, NZ) * NJ + j
    down_z = lax.rem(z + NZ - 1, NZ) * NJ + j
    y_up = lax.rem(y + 1, NY)
    y_far = lax.rem(y + 2, NY)
    y_down = lax.rem(y + 3, NY)
    zdev = ((up_z, y), (down_z, y))
    ydev = ((me, y_up), (me, y_down))

    def peer(o):
        return lax.rem(j + o, NJ)

    def quarter(i):
        return pl.ds(pl.multiple_of((y, y_far, y_down, y_up)[i] * Q, Q), Q)

    halves = [pl.ds(i * (TOK // 2), TOK // 2) for i in range(2)]
    tokens = [
        pltpu.make_async_copy(tok_hbm.at[rows, :], tok_ref.at[rows, :], t_sem.at[i])
        for i, rows in enumerate(halves)
    ]
    for copy in tokens:
        copy.start()

    barrier = pltpu.get_barrier_semaphore()
    partners = list(zdev) + list(ydev) + [(me, y_far)]
    partners += [(z * NJ + peer(o), y) for o in range(1, NJ)]
    for device in partners:
        pl.semaphore_signal(barrier, inc=1, device_id=device, device_id_type=MESH)

    weights = []
    for i in range(4):
        weights.append((wg_ref.at[0, quarter(i), :], wgu.at[pl.ds(i * Q, Q), pl.ds(0, Q)]))
        weights.append((wu_ref.at[0, quarter(i), :], wgu.at[pl.ds(i * Q, Q), pl.ds(Q, Q)]))
        weights.append((wd_ref.at[0, :, quarter(i)], wdn.at[:, pl.ds(i * Q, Q)]))
    weights = [pltpu.make_async_copy(s, d, w_sem.at[i]) for i, (s, d) in enumerate(weights)]

    sends = []

    def send(src, dst, ssem, rsem, device):
        copy = pltpu.make_async_remote_copy(
            src_ref=src, dst_ref=dst, send_sem=ssem, recv_sem=rsem,
            device_id=device, device_id_type=MESH,
        )
        copy.start()
        return copy

    def await_bytes(ref, sem):
        pltpu.make_async_copy(ref, ref, sem).wait()

    ids = ids_ref[...].astype(F32)
    expert = lax.broadcasted_iota(jnp.int32, (NZ * NJ, TOK), 0).astype(F32)
    hits = [ids[k : k + 1, :] == expert for k in range(4)]
    named = jnp.where(hits[0] | hits[1] | hits[2] | hits[3], 1.0, 0.0).astype(BF)
    earlier = lax.broadcasted_iota(jnp.int32, (TOK, TOK), 0) < lax.broadcasted_iota(
        jnp.int32, (TOK, TOK), 1
    )
    before = jnp.dot(named, jnp.where(earlier, 1.0, 0.0).astype(BF), preferred_element_type=F32)
    info_ref[...] = jnp.zeros_like(info_ref)
    info_ref[pl.ds(0, 4), :] = ids
    for k in range(4):
        slot = jnp.sum(jnp.where(hits[k], before, 0.0), axis=0, keepdims=True)
        info_ref[pl.ds(4 + k, 1), :] = slot
    info_ref[pl.ds(8, 4), :] = rw_ref[...]
    za[0, 0, pl.ds(TOK, META), :] = info_ref[...].astype(BF)

    def piece(chunk, b, part):
        rows = TOK + META if (chunk, part) == (A, 0) else TOK
        return (za, zb)[chunk].at[b, part, pl.ds(0, rows), :]

    def z_send(direction, hop, chunk, part):
        here = (-hop if direction == R else hop) % NZ
        there = (-(hop + 1) if direction == R else hop + 1) % NZ
        sends.append(
            send(
                piece(chunk, here, part), piece(chunk, there, part),
                z_s.at[direction, hop, chunk, part], z_r.at[direction, hop, chunk, part],
                zdev[direction],
            )
        )

    def z_step(direction, hop, chunk, part):
        slot = (-hop if direction == R else hop) % NZ
        await_bytes(piece(chunk, slot, part), z_r.at[direction, hop - 1, chunk, part])
        if hop < top_hop(direction, chunk):
            z_send(direction, hop, chunk, part)

    def normalise(chunk, part):
        at = (y, y_far)[chunk] * Q + part * C
        cols = pl.ds(pl.multiple_of(at, C), C)
        for rows, scale in zip(halves, scales):
            value = tok_ref[rows, cols].astype(F32) * scale * gain_ref[:, cols]
            (za, zb)[chunk][0, part, rows, :] = value.astype(BF)

    scales = []
    for copy, rows in zip(tokens, halves):
        copy.wait()
        values = tok_ref[rows, :].astype(F32)
        scales.append(lax.rsqrt(jnp.mean(values * values, axis=1, keepdims=True) + 1e-06))
    for part in range(PARTS):
        normalise(A, part)
        if part == 0:
            pl.semaphore_wait(barrier, len(partners))
        for direction in (R, L):
            z_send(direction, 0, A, part)
    for copy in weights:
        copy.start()
    for part in range(PARTS):
        normalise(B, part)

    def z_start(direction, part):
        z_send(direction, 0, B, part)

    base = (z * ROWS).astype(F32)

    def places(b):
        info = za[b, 0, pl.ds(TOK, META), :].astype(F32)
        row = lax.broadcasted_iota(jnp.int32, (ROWS, TOK), 0)
        row = lax.rem(row, PIECE) // SUB * CAP + row // PIECE * SUB + lax.rem(row, SUB)
        at = row.astype(F32) + base
        return info, [info[k : k + 1] * CAP + info[4 + k : 5 + k] == at for k in range(4)]

    def rows_of(p):
        return pl.ds(pl.multiple_of(p * SUB, SUB), SUB)

    def exchange(src, dst, ssem, rsem):
        for o in (4, 5, 3, 6, 2, 7, 1):
            p = peer(o)
            send(src.at[rows_of(p), :], dst.at[rows_of(j), :], ssem, rsem, (z * NJ + p, y))
        dst[rows_of(j), :] = src[rows_of(j), :]

    def await_exchange(dst, rsem):
        await_bytes(dst.at[pl.ds(0, PIECE - SUB), :], rsem)

    def cut(i):
        return pl.ds(i * PIECE, PIECE)

    def cols(i):
        return pl.ds(i * Q, Q)

    def picked(b, chunk, parts):
        info, at = places(b)
        pick = jnp.where(at[0] | at[1] | at[2] | at[3], 1.0, 0.0).astype(BF)
        for part in parts:
            block = (za, zb)[chunk][b, part, pl.ds(0, TOK), :]
            xs[b, chunk, :, fine(part)] = jnp.dot(
                pick, block, preferred_element_type=F32
            ).astype(BF)

    def fine(part):
        return pl.ds(part * C, C)

    def dispatch(b, chunk):
        picked(b, chunk, range(PARTS))
        exchange(
            xs.at[b, chunk], xf.at[b, :, cols(chunk)], x_s.at[b, chunk, 0], x_r.at[b, chunk, 0]
        )

    def early_dispatch(b, part):
        picked(b, A, (part,))
        exchange(
            xs.at[b, A, :, fine(part)], xf.at[b, :, fine(part)], h_s.at[b, part], h_r.at[b, part]
        )

    def spread(b, i):
        await_exchange(xf.at[b, :, cols(A)], x_r.at[b, A, i])
        for side in range(2):
            sends.append(
                send(
                    xf.at[b, :, cols(A)], xf.at[b, :, cols(2 + side)],
                    y_s.at[side, b, i], y_r.at[side, b, i], ydev[side],
                )
            )

    def early_landing(b, side, part):
        return xf.at[b, :, pl.ds((2 + side) * Q + part * C, C)]

    def early_spread(b, part):
        await_exchange(xf.at[b, :, fine(part)], h_r.at[b, part])
        for side in range(2):
            sends.append(
                send(
                    xf.at[b, :, fine(part)], early_landing(b, side, part),
                    j_s.at[side, b, part], j_r.at[side, b, part], ydev[side],
                )
            )

    def experts(b, i):
        await_exchange(xf.at[b, cut(i), cols(B)], x_r.at[b, B, i])
        for side in range(2):
            if b in EARLY:
                for part in range(PARTS):
                    await_bytes(early_landing(b, side, part), j_r.at[side, b, part])
            else:
                await_bytes(xf.at[b, cut(i), cols(2 + side)], y_r.at[side, b, i])
        rows = xf[b, cut(i), :]
        for n in range(2):
            gate = jnp.dot(rows, wgu[:, pl.ds(n * 256, 256)], preferred_element_type=F32)
            upper = jnp.dot(rows, wgu[:, pl.ds(Q + n * 256, 256)], preferred_element_type=F32)
            gate = jnp.minimum(gate, 7.0)
            upper = jnp.clip(upper, -7.0, 7.0)
            hid[:, pl.ds(n * 256, 256)] = (
                (upper + 1.0) * (gate * jax.nn.sigmoid(1.702 * gate))
            ).astype(BF)
        for q in (2, 3, 1, 0):
            part = jnp.dot(hid[...], wdn[:, cols(q)], preferred_element_type=F32)
            ps[b, q, cut(i), :] = part.astype(BF)
            if q >= 2:
                side = 3 - q
                sends.append(
                    send(
                        ps.at[b, q, cut(i)], yr.at[side, b, cut(i)],
                        p_s.at[side, b, i], p_r.at[side, b, i], ydev[side],
                    )
                )
            elif q == 1:
                exchange(
                    ps.at[b, 1, cut(i)], cr.at[b, B, cut(i)], q_s.at[b, B, i], q_r.at[b, B, i]
                )

    def give_back(b, i):
        total = ps[b, 0, cut(i), :].astype(F32)
        for side in range(2):
            await_bytes(yr.at[side, b, cut(i)], p_r.at[side, b, i])
            total = total + yr[side, b, cut(i), :].astype(F32)
        xs2[b, cut(i), :] = total.astype(BF)
        exchange(xs2.at[b, cut(i)], cr.at[b, A, cut(i)], q_s.at[b, A, i], q_r.at[b, A, i])

    def combine(b, chunk):
        for i in range(CUTS):
            await_exchange(cr.at[b, chunk, cut(i)], q_r.at[b, chunk, i])
        info, at = places(b)
        weight = jnp.zeros((ROWS, TOK), F32)
        for k in range(4):
            weight = jnp.where(at[k], info[8 + k : 9 + k], weight)
        tsum[b, chunk] = lax.dot_general(
            weight.astype(BF), cr[b, chunk], (((0,), (0,)), ((), ())), preferred_element_type=F32
        )

    def span(part):
        return pl.ds(part * (TOK // PARTS), TOK // PARTS)

    def reduce_step(direction, hop, chunk, part):
        b = (hop if direction == R else -hop) % NZ
        value = tsum[b, chunk, span(part), :]
        if hop < top_hop(direction, chunk):
            came = rin.at[direction, hop, chunk, span(part), :]
            await_bytes(came, c_r.at[direction, hop, chunk, part])
            value = value + came[...].astype(F32)
        src = rout.at[direction, hop - 1, chunk, span(part), :]
        src[...] = value.astype(BF)
        sends.append(
            send(
                src, rin.at[direction, hop - 1, chunk, span(part), :],
                c_s.at[direction, hop - 1, chunk, part], c_r.at[direction, hop - 1, chunk, part],
                zdev[direction],
            )
        )

    def arrived(chunk, part):
        total = tsum[0, chunk, span(part), :]
        for direction in (R, L):
            came = rin.at[direction, 0, chunk, span(part), :]
            await_bytes(came, c_r.at[direction, 0, chunk, part])
            total = total + came[...].astype(F32)
        return total

    def finish_far(part):
        exs[span(part), :] = arrived(B, part).astype(BF)
        sends.append(
            send(
                exs.at[span(part), :], far_hbm.at[span(part), :],
                e_s.at[part], e_r.at[part], (me, y_far),
            )
        )

    results = []

    def finish_own(part):
        own_ref[span(part), :] = arrived(A, part)
        copy = pltpu.make_async_copy(
            own_ref.at[span(part), :], own_hbm.at[span(part), :], o_sem.at[part]
        )
        copy.start()
        results.append(copy)

    waiting = list(weights)
    for name in SCHEDULE:
        arg = [int(d) for d in name[1:]]
        if name[0] == "F":
            while waiting:
                waiting.pop().wait()
        {
            "Z": z_step, "D": dispatch, "Y": spread, "F": experts, "G": give_back,
            "C": combine, "r": reduce_step, "B": z_start, "H": early_dispatch, "J": early_spread, "E": finish_far, "O": finish_own,
        }[name[0]](*arg)

    for part in range(PARTS):
        await_bytes(far_hbm.at[span(part), :], e_r.at[part])
    for copy in results:
        copy.wait()
    for copy in sends:
        copy.wait_send()
    for b in range(NZ):
        for i in range(CUTS):
            if b in EARLY:
                for part in range(PARTS):
                    await_exchange(xs.at[b, A, :, fine(part)], h_s.at[b, part])
            else:
                await_exchange(xs.at[b, A], x_s.at[b, A, i])
            await_exchange(xs.at[b, B], x_s.at[b, B, i])
            await_exchange(xs2.at[b, cut(i)], q_s.at[b, A, i])
            await_exchange(ps.at[b, 1, cut(i)], q_s.at[b, B, i])


def per_device(tokens, norm_gain, expert_ids, route_weights, gate_weight, up_weight, down_weight):
    vmem = pl.BlockSpec(memory_space=pltpu.VMEM)
    hbm = pl.BlockSpec(memory_space=pl.ANY)
    dma = pltpu.SemaphoreType.DMA
    own, far = pl.pallas_call(
        kernel,
        out_shape=[jax.ShapeDtypeStruct((TOK, Q), F32), jax.ShapeDtypeStruct((TOK, Q), BF)],
        in_specs=[hbm, vmem, vmem, vmem, hbm, hbm, hbm],
        out_specs=[hbm, hbm],
        scratch_shapes=[
            pltpu.VMEM((TOK, W), BF),
            pltpu.VMEM((TOK, Q), F32),
            pltpu.VMEM((NZ, PARTS, TOK + META, C), BF),
            pltpu.VMEM((NZ, PARTS, TOK, C), BF),
            pltpu.VMEM((NZ, 2, ROWS, Q), BF),
            pltpu.VMEM((NZ, ROWS, W), BF),
            pltpu.VMEM((W, 2 * Q), BF),
            pltpu.VMEM((Q, W), BF),
            pltpu.VMEM((PIECE, Q), BF),
            pltpu.VMEM((NZ, 4, ROWS, Q), BF),
            pltpu.VMEM((2, NZ, ROWS, Q), BF),
            pltpu.VMEM((NZ, ROWS, Q), BF),
            pltpu.VMEM((NZ, 2, ROWS, Q), BF),
            pltpu.VMEM((NZ, 2, TOK, Q), F32),
            pltpu.VMEM((2, HALF, 2, TOK, Q), BF),
            pltpu.VMEM((2, HALF, 2, TOK, Q), BF),
            pltpu.VMEM((TOK, Q), BF),
            pltpu.VMEM((META, TOK), F32),
            dma((2,)), dma((PARTS,)),
            dma((NZ, PARTS)), dma((NZ, PARTS)),
            dma((2, NZ, PARTS)), dma((2, NZ, PARTS)),
            dma((12,)),
            dma((2, HALF, 2, PARTS)), dma((2, HALF, 2, PARTS)),
            dma((NZ, 2, CUTS)), dma((NZ, 2, CUTS)),
            dma((2, NZ, CUTS)), dma((2, NZ, CUTS)),
            dma((2, NZ, CUTS)), dma((2, NZ, CUTS)),
            dma((NZ, 2, CUTS)), dma((NZ, 2, CUTS)),
            dma((2, HALF, 2, PARTS)), dma((2, HALF, 2, PARTS)),
            dma((PARTS,)), dma((PARTS,)),
        ],
        compiler_params=pltpu.CompilerParams(
            collective_id=0, has_side_effects=True, vmem_limit_bytes=67_000_000
        ),
        name="moe",
    )(
        tokens, norm_gain.reshape(1, W), expert_ids.T, route_weights.T,
        gate_weight, up_weight, down_weight,
    )
    return (own + far.astype(F32)).astype(BF)


def solution(mesh):
    in_specs = (
        P("ep", None),
        P(),
        P("ep", None),
        P("ep", None),
        P("ep", None, "tp"),
        P("ep", None, "tp"),
        P("ep", "tp", None),
    )
    out_specs = P("ep", "tp")
    return jax.shard_map(
        per_device, mesh=mesh, in_specs=in_specs, out_specs=out_specs, check_vma=False
    )
```
